32 devices in a mesh: sp: 8 (over z, y), tp: 4 (over x, core).
Axes of the slice: x: 2, y: 2, z: 4, core: 2. Of those that a mesh axis runs over, the one named last changes fastest.
Arguments:
- tokens: bfloat16 [1024, 2048], P(('sp', 'tp')), may hold values from -6 to 6
- doc_lengths: int32 [16], replicated, may hold values from 1 to 640, 1024 in all
- query_down: bfloat16 [2048, 512], replicated, may hold values from -0.125 to 0.125
- latent_down: bfloat16 [2048, 256], replicated, may hold values from -0.125 to 0.125
- rope_down: bfloat16 [2048, 32], replicated, may hold values from -0.125 to 0.125
- query_latent_gain: float32 [512], replicated, may hold values from 0.1 to 1.9
- latent_gain: float32 [256], replicated, may hold values from 0.1 to 1.9
- query_up: bfloat16 [512, 768], P(None, 'tp'), may hold values from -0.25 to 0.25
- key_up: bfloat16 [256, 512], P(None, 'tp'), may hold values from -0.375 to 0.375
- value_up: bfloat16 [256, 512], P(None, 'tp'), may hold values from -0.375 to 0.375
- query_gain: float32 [96], replicated, may hold values from 0.5 to 15
- key_gain: float32 [96], replicated, may hold values from 0.5 to 15
- output_gain: float32 [512], replicated, may hold values from 0.1 to 1.9
- output_weight: bfloat16 [512, 2048], P(None, 'tp'), may hold values from -0.25 to 0.25
Outputs:
- layer_output: bfloat16 [1024, 2048], P('sp', 'tp')
- log_totals: float32 [8, 1024], P('tp', 'sp')
The draws below stay inside these ranges and needn't reach their ends.
Inputs may be any that keep to these rules, and one draw needn't show every extreme that they name: `doc_lengths`: the lengths sum to 1024; the longest is exactly 640.
All inputs are finite; a program needn't handle non-finite values.
Results may differ from the reference program's by a relative error of at most 0.019.
The reference program's roundings to bfloat16 on the way count: a program that leaves them out, or rounds other values in their place, can miss the bound.
Values may be sent and summed in bfloat16 or wider, within the bound.
A program may use at most 64 MiB of HBM per device.

```python
import math
import jax
import jax.numpy as jnp
import numpy as np
from jax import lax

D = 2048
QR = 512
KVR = 256
H = 8
NOPE = 64
ROPE = 32
VD = 64
NDOC = 16
SEQ = 1024


def gain_table(key, salt_value):
    gains_out = jax.random.uniform(jax.random.fold_in(key, salt_value), (NOPE + ROPE,), jnp.float32, 0.5, 1.5)
    return gains_out


def draw_query_gain(key, part):
    return gain_table(key, 101)


def draw_key_gain(key, part):
    return gain_table(key, 202)


def block_scale(key, dims, split, least, top_value):
    gain = 1.0
    for position, shards_of in split:
        draws = jax.random.uniform(jax.random.fold_in(jax.random.fold_in(key, 6), position), (shards_of,), jnp.float32, least / len(split), top_value / len(split))
        gain = gain * jnp.repeat(jnp.exp(draws), dims[position] // shards_of).reshape((-1,) + (1,) * (len(dims) - 1 - position))
    return gain


def length_profile(amount, total, most, lean):
    weights = [(1 << 20) // math.isqrt(standing ** lean) + 1 for standing in range(2, amount + 1)]
    rest, given = total - most - (amount - 1), [1] * (amount - 1)
    while rest > 0:
        candidates = [i for i in range(amount - 1) if given[i] < most]
        mass, remaining = sum([weights[i] for i in candidates]), rest
        for i in candidates:
            addition = min(most - given[i], max(1, remaining * weights[i] // mass), rest)
            given[i] = given[i] + addition
            rest = rest - addition
    return np.array([most] + given)


def uneven(own_key, amount, total, most, lean):
    if amount == 2:
        one = jax.random.randint(own_key, (), max(1, total - most), min(most, total - 1) + 1)
        return jnp.stack([one, total - one])
    tallies = jnp.asarray(length_profile(amount, total, most, lean), jnp.int32)
    pairs = (amount - 1) // 2
    giver, taker = tallies[1:1 + 2 * pairs:2], tallies[2:2 + 2 * pairs:2]
    margin = jnp.minimum(giver - 1, most - taker)
    shifted = jax.random.randint(jax.random.fold_in(own_key, 1), (pairs,), 0, 1 << 20) % (margin + 1)
    tallies = tallies.at[1:1 + 2 * pairs:2].set(giver - shifted).at[2:2 + 2 * pairs:2].set(taker + shifted)
    return tallies[jax.random.permutation(jax.random.fold_in(own_key, 2), amount)]


def normal_values(own_key, shape, scale, limit, shards=(), kind=jnp.bfloat16):
    level = block_scale(own_key, shape, shards, -0.22, 0.18) if shards else 1.0
    values = jax.random.normal(own_key, shape, jnp.float32) * scale * level
    return jnp.minimum(jnp.maximum(values, -limit), limit).astype(kind)


def setup_inputs(seed: int = 0) -> dict:
    keys = jax.random.split(jax.random.key(seed), 15)
    return {
        "tokens": normal_values(keys[0], (SEQ, D), 1.0, 6.0, ((0, 32),)),
        "doc_lengths": uneven(keys[1], NDOC, SEQ, SEQ * 5 // 8, 2).astype(jnp.int32),
        "query_down": normal_values(keys[2], (D, QR), D ** -0.5, 0.125),
        "latent_down": normal_values(keys[3], (D, KVR), D ** -0.5, 0.125),
        "rope_down": normal_values(keys[4], (D, ROPE), D ** -0.5, 0.125),
        "query_latent_gain": jnp.clip(1.0 + 0.18 * jax.random.normal(keys[5], (QR,), jnp.float32), 0.1, 1.9),
        "latent_gain": jnp.clip(1.0 + 0.18 * jax.random.normal(keys[6], (KVR,), jnp.float32), 0.1, 1.9),
        "query_up": normal_values(keys[7], (QR, H * (NOPE + ROPE)), QR ** -0.5, 0.25, ((1, 4),)),
        "key_up": normal_values(keys[8], (KVR, H * NOPE), KVR ** -0.5, 0.375, ((1, 4),)),
        "value_up": normal_values(keys[9], (KVR, H * VD), KVR ** -0.5, 0.375, ((1, 4),)),
        "query_gain": draw_query_gain(jax.random.fold_in(keys[14], 71), 0),
        "key_gain": draw_key_gain(jax.random.fold_in(keys[14], 71), 0),
        "output_gain": jnp.clip(1.0 + 0.18 * jax.random.normal(keys[12], (H * VD,), jnp.float32), 0.1, 1.9),
        "output_weight": normal_values(keys[13], (H * VD, D), (H * VD) ** -0.5, 0.25, ((1, 4),)),
    }


EPS = 1e-06
THETA = 10000.0
NEG = -1e+30

def norm_rows(matrix, scaling):
    mean_square = lax.optimization_barrier(jnp.mean(matrix * matrix, axis=-1, keepdims=True))
    return matrix * lax.rsqrt(mean_square + EPS) * scaling

def rotate(matrix, places):
    half_width = matrix.shape[-1] // 2
    inverse = THETA ** (-jnp.arange(half_width, dtype=jnp.float32) / half_width)
    angles = places.astype(jnp.float32)[:, None, None] * inverse
    cosine = jnp.cos(angles)
    sine_part = jnp.sin(angles)
    leading = matrix[..., :half_width]
    trailing = matrix[..., half_width:]
    return jnp.concatenate([leading * cosine - trailing * sine_part, trailing * cosine + leading * sine_part], axis=-1)

def doc_index(places, doc_ends):
    return lax.optimization_barrier(jnp.sum((places[:, None] >= doc_ends[None, :]).astype(jnp.int32), axis=1)).astype(jnp.int32)

def head_keys(latent_rows, rope_rows, places, key_up, value_up, key_gain):
    row_count = latent_rows.shape[0]
    head_count = key_up.shape[1] // NOPE
    plain_part = jnp.dot(latent_rows, key_up, preferred_element_type=jnp.float32).reshape(row_count, head_count, NOPE)
    shared_part = jnp.broadcast_to(rope_rows.astype(jnp.float32)[:, None, :], (row_count, head_count, ROPE))
    joined = norm_rows(jnp.concatenate([plain_part, shared_part], axis=-1), key_gain)
    key_block = jnp.concatenate([joined[..., :NOPE], rotate(joined[..., NOPE:], places)], axis=-1).astype(jnp.bfloat16)
    value_block = jnp.dot(latent_rows, value_up, preferred_element_type=jnp.float32).astype(jnp.bfloat16)
    return (key_block, value_block.reshape(row_count, head_count, VD))

def reference(tokens, doc_lengths, query_down, latent_down, rope_down, query_latent_gain, latent_gain, query_up, key_up, value_up, query_gain, key_gain, output_gain, output_weight):
    head_width = NOPE + ROPE
    query_latent = norm_rows(jnp.dot(tokens, query_down, preferred_element_type=jnp.float32), query_latent_gain).astype(jnp.bfloat16)
    key_latent = norm_rows(jnp.dot(tokens, latent_down, preferred_element_type=jnp.float32), latent_gain).astype(jnp.bfloat16)
    rope_key = jnp.dot(tokens, rope_down, preferred_element_type=jnp.float32).astype(jnp.bfloat16)
    places = jnp.arange(SEQ, dtype=jnp.int32)
    doc_ends = jnp.cumsum(doc_lengths).astype(jnp.int32)
    docs = doc_index(places, doc_ends)
    query_raw = jnp.dot(query_latent, query_up, preferred_element_type=jnp.float32).reshape(SEQ, H, head_width)
    query_raw = norm_rows(query_raw, query_gain)
    queries = jnp.concatenate([query_raw[..., :NOPE], rotate(query_raw[..., NOPE:], places)], axis=-1).astype(jnp.bfloat16)
    key_block, value_block = head_keys(key_latent, rope_key, places, key_up, value_up, key_gain)
    keys_wide = key_block.astype(jnp.float32)
    values_wide = value_block.astype(jnp.float32)
    block_rows = math.gcd(SEQ, 512)
    block_count = SEQ // block_rows
    score_scale = head_width ** (-0.5)

    def one_block(block_index):
        begin_at = (block_index * block_rows).astype(jnp.int32)
        query_part = lax.dynamic_slice_in_dim(queries, begin_at, block_rows, 0).astype(jnp.float32)
        query_docs = lax.dynamic_slice_in_dim(docs, begin_at, block_rows, 0)
        scores = jnp.einsum('qhd,khd->hqk', query_part, keys_wide) * score_scale
        allowed = (query_docs[:, None] == docs[None, :])[None]
        scores = jnp.where(allowed, scores, NEG)
        row_top = lax.optimization_barrier(jnp.max(scores, axis=-1))
        expd_part = jnp.where(allowed, jnp.exp(scores - row_top[..., None]), 0.0)
        row_total = lax.optimization_barrier(jnp.sum(expd_part, axis=-1))
        weights = lax.optimization_barrier(expd_part.astype(jnp.bfloat16)).astype(jnp.float32)
        weighted = jnp.einsum('hqk,khd->qhd', weights, values_wide)
        head_out = (weighted / jnp.transpose(row_total)[:, :, None]).astype(jnp.bfloat16)
        return (head_out, row_top + jnp.log(row_total))
    head_blocks, log_blocks = lax.map(one_block, jnp.arange(block_count, dtype=jnp.int32))
    head_out = head_blocks.reshape(SEQ, H * VD)
    log_totals = jnp.transpose(log_blocks, (1, 0, 2)).reshape(H, SEQ)
    normed = norm_rows(head_out.astype(jnp.float32), output_gain).astype(jnp.bfloat16)
    layer_output = jnp.dot(normed, output_weight, preferred_element_type=jnp.float32).astype(jnp.bfloat16)
    return (layer_output, log_totals)
```

```python
import functools

import jax
import jax.numpy as jnp
import numpy as np
from jax import lax
from jax.experimental import pallas as pl
from jax.experimental.pallas import tpu as pltpu
from jax.sharding import PartitionSpec as P

NOPE = 64
ROPE = 32
VD = 64
WIDTH = NOPE + ROPE
LANES = 128

EPS = 1e-06
THETA = 10000.0
NEG = -1e30
KEY_CHUNK = 1024
F32 = jnp.float32
BF16 = jnp.bfloat16
MESH = pl.DeviceIdType.MESH


def each(count, body):
    if count <= 16:
        for step in range(count):
            body(step)
    else:
        lax.fori_loop(0, count, lambda step, _: (body(step), 0)[1], 0)


def nt_dot(left, right):
    return lax.dot_general(left, right, (((1,), (1,)), ((), ())), preferred_element_type=F32)


def norm_lanes(matrix, scaling):
    mean_square = jnp.mean(matrix * matrix, axis=-1, keepdims=True)
    return matrix * lax.rsqrt(mean_square + EPS) * scaling


def column(row):
    width = row.shape[1]
    full = jnp.broadcast_to(row, (LANES, width))
    full = jnp.concatenate([full, jnp.zeros((LANES, LANES - width), F32)], axis=1)
    return jnp.transpose(full)[:width, 0:1]


def rotated(part, cosine, sine):
    half = part.shape[0] // 2
    leading, trailing = part[:half], part[half:]
    return jnp.concatenate(
        [leading * cosine - trailing * sine, trailing * cosine + leading * sine], axis=0
    )


def xor(index, bits):
    return jnp.bitwise_xor(index, bits)


def kernel(
    n_sp, n_tp,
    tokens_hbm, lengths_hbm, query_down_hbm, latent_down_hbm, rope_down_hbm,
    query_latent_gain_hbm, latent_gain_hbm, query_up_hbm, key_up_hbm, value_up_hbm,
    query_gain_hbm, key_gain_hbm, output_gain_hbm, output_weight_hbm, inverse_hbm,
    out_ref, log_ref,
    tokens, lengths, query_down, latent_down, rope_down,
    query_latent_gain, latent_gain, query_up, key_up, value_up,
    query_gain, key_gain, output_gain, output_weight, inverse_ref,
    lat, qlat, heads, load_sem,
    z_send, z_recv, a_send, a_recv, b_send, b_recv, c_send, c_recv,
    q_send, q_recv, h_send, h_recv,
):
    sp, tp = lax.axis_index("sp"), lax.axis_index("tp")
    n_outer = n_sp // 2
    rows = tokens.shape[0]
    group_rows = rows * n_tp
    kvr = latent_down.shape[1]
    head_count = key_up.shape[1] // NOPE
    out_width = head_count * VD

    loads = [
        pltpu.make_async_copy(source, target, load_sem.at[position])
        for position, (source, target) in enumerate((
            (tokens_hbm, tokens), (latent_down_hbm, latent_down), (rope_down_hbm, rope_down),
            (latent_gain_hbm, latent_gain), (query_down_hbm, query_down),
            (query_latent_gain_hbm, query_latent_gain), (lengths_hbm, lengths),
            (query_gain_hbm, query_gain), (key_gain_hbm, key_gain), (inverse_hbm, inverse_ref),
            (query_up_hbm, query_up), (key_up_hbm, key_up), (value_up_hbm, value_up),
            (output_gain_hbm, output_gain), (output_weight_hbm, output_weight),
        ))
    ]
    for load in loads:
        load.start()

    barrier = pltpu.get_barrier_semaphore()

    def greet(step):
        pl.semaphore_signal(
            barrier, inc=1, device_id=(xor(sp, 2 * (step + 1)), tp), device_id_type=MESH
        )

    each(n_outer - 1, greet)
    pl.semaphore_signal(barrier, inc=1, device_id=(xor(sp, 1), tp), device_id_type=MESH)
    for other in range(1, n_tp):
        pl.semaphore_signal(barrier, inc=1, device_id=(sp, xor(tp, other)), device_id_type=MESH)

    parity = lax.rem(tp, 2)
    first = (xor(sp, 1 - parity), xor(tp, 2 * parity))
    second = (xor(sp, parity), xor(tp, 2 * (1 - parity)))
    core = (sp, xor(tp, 1))

    def block(device):
        start = pl.multiple_of((device[0] * n_tp + device[1]) * rows, rows)
        return lat.at[pl.ds(start, rows)]

    def send(ref, sends, recvs, index, target):
        copy = pltpu.make_async_remote_copy(
            src_ref=ref, dst_ref=ref, send_sem=sends.at[index], recv_sem=recvs.at[index],
            device_id=target, device_id_type=MESH,
        )
        copy.start()
        return copy

    def along(device, step):
        return (xor(device[0], 2 * step), device[1])

    me = (sp, tp)
    for load in loads[:4]:
        load.wait()
    latent = jnp.dot(tokens[...], latent_down[...], preferred_element_type=F32)
    rope = jnp.dot(tokens[...], rope_down[...], preferred_element_type=F32)
    latent = norm_lanes(latent, latent_gain[...]).astype(BF16)
    rope = jnp.concatenate([rope, jnp.zeros((rows, LANES - ROPE), F32)], axis=1).astype(BF16)
    own = pl.ds(pl.multiple_of((sp * n_tp + tp) * rows, rows), rows)
    lat[own, :kvr] = latent
    lat[own, kvr:] = rope
    pl.semaphore_wait(barrier, n_outer + n_tp - 1)

    each(n_outer - 1, lambda k: send(block(me), z_send, z_recv, k, along(me, k + 1)) and None)
    send(block(me), a_send, a_recv, 0, first)
    send(block(me), b_send, b_recv, 0, second)
    send(block(me), c_send, c_recv, 0, core)

    for load in loads[4:6]:
        load.wait()
    query_latent = jnp.dot(tokens[...], query_down[...], preferred_element_type=F32)
    query_latent = norm_lanes(query_latent, query_latent_gain[...]).astype(BF16)
    own_q = pl.ds(pl.multiple_of(tp * rows, rows), rows)
    qlat[own_q, :] = query_latent
    for other in range(1, n_tp):
        send(qlat.at[own_q], q_send, q_recv, other - 1, (sp, xor(tp, other)))

    for load in loads[6:]:
        load.wait()
    inverse = inverse_ref[...]
    query_gain_column = column(query_gain[...])
    key_gain_column = column(key_gain[...])
    ends = []
    total = 0
    for doc in range(lengths.shape[0]):
        total = total + lengths[doc]
        ends.append(total)

    def docs_of(places):
        found = jnp.zeros(places.shape, jnp.int32)
        for end in ends:
            found = found + (places >= end).astype(jnp.int32)
        return found

    seq = lat.shape[0]
    span = min(seq, KEY_CHUNK)
    query_base = sp * group_rows
    query_places = query_base + lax.broadcasted_iota(jnp.int32, (1, group_rows), 1)
    query_angles = inverse * query_places.astype(F32)
    query_cos, query_sin = jnp.cos(query_angles), jnp.sin(query_angles)
    query_docs = docs_of(query_base + lax.broadcasted_iota(jnp.int32, (group_rows, 1), 0))

    def key_tables(offset):
        places = offset + lax.broadcasted_iota(jnp.int32, (1, span), 1)
        angles = inverse * places.astype(F32)
        return jnp.cos(angles), jnp.sin(angles), docs_of(places) == query_docs

    plain_rows = head_count * NOPE
    key_up_t = jnp.transpose(key_up[...].astype(F32)).astype(BF16)
    eye = (
        lax.broadcasted_iota(jnp.int32, (ROPE, LANES), 0)
        == lax.broadcasted_iota(jnp.int32, (ROPE, LANES), 1)
    ).astype(F32).astype(BF16)
    if seq == span:
        tables = key_tables(0)

    def recv(ref, sends, recvs, index, target):
        pltpu.make_async_remote_copy(
            src_ref=ref, dst_ref=ref, send_sem=sends.at[index], recv_sem=recvs.at[index],
            device_id=target, device_id_type=MESH,
        ).wait_recv()

    def from_first(k):
        source = along(first, k)
        recv(block(source), a_send, a_recv, k, first)
        send(block(source), b_send, b_recv, 2 * k + 1, second)
        send(block(source), c_send, c_recv, 4 * k + 1, core)

    def from_z(k):
        source = along(me, k)
        recv(block(source), z_send, z_recv, k - 1, source)
        send(block(source), a_send, a_recv, k, first)
        send(block(source), b_send, b_recv, 2 * k, second)
        send(block(source), c_send, c_recv, 4 * k, core)

    def both(k):
        return along((xor(sp, 1), xor(tp, 2)), k)

    def from_second(k):
        source = along(second, k)
        recv(block(source), b_send, b_recv, 2 * k, second)
        send(block(source), c_send, c_recv, 4 * k + 2, core)

    def from_both(k):
        source = both(k)
        recv(block(source), b_send, b_recv, 2 * k + 1, second)
        send(block(source), c_send, c_recv, 4 * k + 3, core)

    from_first(0)
    from_second(0)
    each(n_outer - 1, lambda k: from_z(k + 1))
    from_both(0)

    def rest(k):
        from_first(k + 1)
        from_second(k + 1)

    each(n_outer - 1, rest)

    for other in range(1, n_tp):
        peer = xor(tp, other)
        rows_of = pl.ds(pl.multiple_of(peer * rows, rows), rows)
        recv(qlat.at[rows_of], q_send, q_recv, other - 1, (sp, peer))
    raw = jnp.dot(qlat[...], query_up[...], preferred_element_type=F32)
    queries = []
    for head in range(head_count):
        piece = raw[:, head * WIDTH:(head + 1) * WIDTH]
        piece = jnp.concatenate([piece, jnp.zeros((group_rows, LANES - WIDTH), F32)], axis=1)
        piece = jnp.transpose(piece)[:WIDTH]
        scale = lax.rsqrt(jnp.mean(piece * piece, axis=0, keepdims=True) + EPS)
        piece = piece * scale * query_gain_column
        piece = jnp.concatenate(
            [piece[:NOPE], rotated(piece[NOPE:], query_cos, query_sin),
             jnp.zeros((LANES - WIDTH, group_rows), F32)], axis=0
        )
        queries.append(jnp.transpose(piece)[:, :WIDTH].astype(BF16))

    each(n_outer - 1, lambda k: from_both(k + 1))

    def from_core(k):
        recv(block(along(core, k)), c_send, c_recv, 4 * k, core)
        partner_first = (xor(core[0], parity), xor(core[1], 2 * (1 - parity)))
        partner_second = (xor(core[0], 1 - parity), xor(core[1], 2 * parity))
        recv(block(along(partner_first, k)), c_send, c_recv, 4 * k + 1, core)
        recv(block(along(partner_second, k)), c_send, c_recv, 4 * k + 2, core)
        recv(block(along((xor(core[0], 1), xor(core[1], 2)), k)), c_send, c_recv, 4 * k + 3, core)

    each(n_outer, from_core)

    lane = lax.broadcasted_iota(jnp.int32, (group_rows, out_width), 1)
    score_scale = WIDTH ** (-0.5)

    def absorb(offset, known, carried):
        cosine, sine, allowed = known
        block_rows = lat[pl.ds(offset, span), :]
        latents = block_rows[:, :kvr]
        plain = nt_dot(key_up_t, latents)
        shared = nt_dot(eye, block_rows[:, kvr:])
        values = jnp.dot(latents, value_up[...], preferred_element_type=F32).astype(BF16)
        shared_square = jnp.sum(shared * shared, axis=0, keepdims=True)
        fresh = []
        for head in range(head_count):
            top, row_total, weighted = carried[head]
            part = plain[head * NOPE:(head + 1) * NOPE]
            square = jnp.sum(part * part, axis=0, keepdims=True) + shared_square
            scale = lax.rsqrt(square * (1.0 / WIDTH) + EPS)
            tail = rotated(shared * scale * key_gain_column[NOPE:], cosine, sine)
            keys = jnp.concatenate(
                [part * scale * key_gain_column[:NOPE], tail], axis=0
            ).astype(BF16)
            scores = jnp.dot(queries[head], keys, preferred_element_type=F32) * score_scale
            scores = jnp.where(allowed, scores, NEG)
            newest = jnp.maximum(top, jnp.max(scores, axis=1, keepdims=True))
            weights = jnp.where(allowed, jnp.exp(scores - newest), 0.0)
            rescale = jnp.exp(top - newest)
            row_total = row_total * rescale + jnp.sum(weights, axis=1, keepdims=True)
            weighted = weighted * rescale + jnp.dot(
                weights.astype(BF16), values, preferred_element_type=F32
            )
            fresh.append((newest, row_total, weighted))
        return tuple(fresh)

    carried = tuple(
        (jnp.full((group_rows, 1), NEG, F32), jnp.zeros((group_rows, 1), F32),
         jnp.zeros((group_rows, out_width), F32))
        for _ in range(head_count)
    )
    if seq == span:
        carried = absorb(0, tables, carried)
    else:
        def one_chunk(turn, held):
            offset = pl.multiple_of(turn * span, span)
            return absorb(offset, key_tables(offset), held)

        carried = lax.fori_loop(0, seq // span, one_chunk, carried)

    head_out = jnp.zeros((group_rows, out_width), F32)
    for head in range(head_count):
        top, row_total, weighted = carried[head]
        inside = (lane >= head * VD) & (lane < (head + 1) * VD)
        head_out = jnp.where(inside, weighted / row_total, head_out)
    heads[tp] = head_out.astype(BF16)
    for other in range(1, n_tp):
        send(heads.at[tp], h_send, h_recv, other - 1, (sp, xor(tp, other)))

    logs = jnp.concatenate(
        [jnp.broadcast_to(top + jnp.log(row_total), (group_rows, LANES // head_count))
         for top, row_total, _ in carried], axis=1
    )
    logs = jnp.transpose(logs)
    for head in range(head_count):
        start = head * (LANES // head_count)
        log_ref[head:head + 1, :] = logs[start:start + 1]

    for other in range(1, n_tp):
        peer = xor(tp, other)
        recv(heads.at[peer], h_send, h_recv, other - 1, (sp, peer))
    pieces = [heads[index].astype(F32) for index in range(n_tp)]
    square = sum(jnp.sum(piece * piece, axis=1, keepdims=True) for piece in pieces)
    scale = lax.rsqrt(square * (1.0 / (n_tp * out_width)) + EPS)
    normed = jnp.concatenate(
        [(piece * scale * output_gain[:, index * out_width:(index + 1) * out_width]).astype(BF16)
         for index, piece in enumerate(pieces)], axis=1
    )
    out_ref[...] = jnp.dot(normed, output_weight[...], preferred_element_type=F32).astype(BF16)

    def sent(ref, sends, recvs, index):
        pltpu.make_async_remote_copy(
            src_ref=ref, dst_ref=ref, send_sem=sends.at[index], recv_sem=recvs.at[index],
            device_id=core, device_id_type=MESH,
        ).wait_send()

    each(n_outer - 1, lambda k: sent(block(me), z_send, z_recv, k))
    each(n_outer, lambda k: sent(block(along(me, k)), a_send, a_recv, k))

    def sent_rest(k):
        sent(block(along(me, k)), b_send, b_recv, 2 * k)
        sent(block(along(first, k)), b_send, b_recv, 2 * k + 1)
        sent(block(along(me, k)), c_send, c_recv, 4 * k)
        sent(block(along(first, k)), c_send, c_recv, 4 * k + 1)
        sent(block(along(second, k)), c_send, c_recv, 4 * k + 2)
        sent(block(both(k)), c_send, c_recv, 4 * k + 3)

    each(n_outer, sent_rest)
    for other in range(n_tp - 1):
        sent(qlat.at[own_q], q_send, q_recv, other)
        sent(heads.at[tp], h_send, h_recv, other)


def per_device(
    n_sp, n_tp, tokens, doc_lengths, query_down, latent_down, rope_down,
    query_latent_gain, latent_gain, query_up, key_up, value_up,
    query_gain, key_gain, output_gain, output_weight,
):
    rows = tokens.shape[0]
    group_rows = rows * n_tp
    seq = group_rows * n_sp
    half = ROPE // 2
    inverse = jnp.asarray(
        np.float32(THETA) ** (-np.arange(half, dtype=np.float32) / half), F32
    ).reshape(half, 1)
    operands = (
        tokens, doc_lengths, query_down, latent_down, rope_down,
        query_latent_gain[None], latent_gain[None], query_up, key_up, value_up,
        query_gain[None], key_gain[None], output_gain[None], output_weight, inverse,
    )
    n_outer = n_sp // 2
    head_count = key_up.shape[1] // NOPE
    kvr = latent_down.shape[1]
    held = [
        pltpu.SMEM(member.shape, member.dtype) if position == 1
        else pltpu.VMEM(member.shape, member.dtype)
        for position, member in enumerate(operands)
    ]
    dma = pltpu.SemaphoreType.DMA
    return pl.pallas_call(
        functools.partial(kernel, n_sp, n_tp),
        out_shape=(
            jax.ShapeDtypeStruct((group_rows, output_weight.shape[1]), BF16),
            jax.ShapeDtypeStruct((head_count, group_rows), F32),
        ),
        in_specs=[pl.BlockSpec(memory_space=pl.ANY)] * len(operands),
        out_specs=(pl.BlockSpec(memory_space=pltpu.VMEM),) * 2,
        scratch_shapes=held + [
            pltpu.VMEM((seq, kvr + LANES), BF16),
            pltpu.VMEM((group_rows, query_down.shape[1]), BF16),
            pltpu.VMEM((n_tp, group_rows, head_count * VD), BF16),
            dma((len(operands),)),
            dma((n_outer - 1,)), dma((n_outer - 1,)),
            dma((n_outer,)), dma((n_outer,)),
            dma((2 * n_outer,)), dma((2 * n_outer,)),
            dma((4 * n_outer,)), dma((4 * n_outer,)),
            dma((n_tp - 1,)), dma((n_tp - 1,)),
            dma((n_tp - 1,)), dma((n_tp - 1,)),
        ],
        compiler_params=pltpu.CompilerParams(
            collective_id=0, has_side_effects=True, vmem_limit_bytes=60 * 1024 * 1024
        ),
    )(*operands)


def solution(mesh):
    n_sp, n_tp = mesh.shape["sp"], mesh.shape["tp"]
    return jax.shard_map(
        functools.partial(per_device, n_sp, n_tp),
        mesh=mesh,
        in_specs=(
            P(("sp", "tp"), None), P(), P(), P(), P(), P(), P(),
            P(None, "tp"), P(None, "tp"), P(None, "tp"),
            P(), P(), P(), P(None, "tp"),
        ),
        out_specs=(P("sp", "tp"), P("tp", "sp")),
        check_vma=False,
    )
```

```python
import functools

import jax
import jax.numpy as jnp
import numpy as np
from jax import lax
from jax.experimental import pallas as pl
from jax.experimental.pallas import tpu as pltpu
from jax.sharding import PartitionSpec as P

NOPE = 64
ROPE = 32
VD = 64
WIDTH = NOPE + ROPE
LANES = 128

EPS = 1e-06
THETA = 10000.0
NEG = -1e30
KEY_CHUNK = 1024
F32 = jnp.float32
BF16 = jnp.bfloat16
MESH = pl.DeviceIdType.MESH


def each(count, body):
    if count <= 16:
        for step in range(count):
            body(step)
    else:
        lax.fori_loop(0, count, lambda step, _: (body(step), 0)[1], 0)


def nt_dot(left, right):
    return lax.dot_general(left, right, (((1,), (1,)), ((), ())), preferred_element_type=F32)


def norm_lanes(matrix, scaling):
    mean_square = jnp.mean(matrix * matrix, axis=-1, keepdims=True)
    return matrix * lax.rsqrt(mean_square + EPS) * scaling


def column(row):
    width = row.shape[1]
    full = jnp.broadcast_to(row, (LANES, width))
    full = jnp.concatenate([full, jnp.zeros((LANES, LANES - width), F32)], axis=1)
    return jnp.transpose(full)[:width, 0:1]


def rotated(part, cosine, sine):
    half = part.shape[0] // 2
    leading, trailing = part[:half], part[half:]
    return jnp.concatenate(
        [leading * cosine - trailing * sine, trailing * cosine + leading * sine], axis=0
    )


def xor(index, bits):
    return jnp.bitwise_xor(index, bits)


def kernel(
    n_sp, n_tp,
    tokens_hbm, lengths_hbm, query_down_hbm, latent_down_hbm, rope_down_hbm,
    query_latent_gain_hbm, latent_gain_hbm, query_up_hbm, key_up_hbm, value_up_hbm,
    query_gain_hbm, key_gain_hbm, output_gain_hbm, output_weight_hbm, inverse_hbm,
    out_ref, log_ref,
    tokens, lengths, query_down, latent_down, rope_down,
    query_latent_gain, latent_gain, query_up, key_up, value_up,
    query_gain, key_gain, output_gain, output_weight, inverse_ref,
    lat, qlat, heads, load_sem,
    z_send, z_recv, a_send, a_recv, b_send, b_recv, c_send, c_recv,
    q_send, q_recv, h_send, h_recv,
):
    sp, tp = lax.axis_index("sp"), lax.axis_index("tp")
    n_outer = n_sp // 2
    rows = tokens.shape[0]
    group_rows = rows * n_tp
    kvr = latent_down.shape[1]
    head_count = key_up.shape[1] // NOPE
    out_width = head_count * VD

    loads = [
        pltpu.make_async_copy(source, target, load_sem.at[position])
        for position, (source, target) in enumerate((
            (tokens_hbm, tokens), (latent_down_hbm, latent_down), (rope_down_hbm, rope_down),
            (latent_gain_hbm, latent_gain), (query_down_hbm, query_down),
            (query_latent_gain_hbm, query_latent_gain), (lengths_hbm, lengths),
            (query_gain_hbm, query_gain), (key_gain_hbm, key_gain), (inverse_hbm, inverse_ref),
            (query_up_hbm, query_up), (key_up_hbm, key_up), (value_up_hbm, value_up),
            (output_gain_hbm, output_gain), (output_weight_hbm, output_weight),
        ))
    ]
    for load in loads:
        load.start()

    barrier = pltpu.get_barrier_semaphore()

    def greet(step):
        pl.semaphore_signal(
            barrier, inc=1, device_id=(xor(sp, 2 * (step + 1)), tp), device_id_type=MESH
        )

    each(n_outer - 1, greet)
    pl.semaphore_signal(barrier, inc=1, device_id=(xor(sp, 1), tp), device_id_type=MESH)
    for other in range(1, n_tp):
        pl.semaphore_signal(barrier, inc=1, device_id=(sp, xor(tp, other)), device_id_type=MESH)

    parity = lax.rem(tp, 2)
    first = (xor(sp, 1 - parity), xor(tp, 2 * parity))
    second = (xor(sp, parity), xor(tp, 2 * (1 - parity)))
    core = (sp, xor(tp, 1))

    def block(device):
        start = pl.multiple_of((device[0] * n_tp + device[1]) * rows, rows)
        return lat.at[pl.ds(start, rows)]

    def send(ref, sends, recvs, index, target):
        copy = pltpu.make_async_remote_copy(
            src_ref=ref, dst_ref=ref, send_sem=sends.at[index], recv_sem=recvs.at[index],
            device_id=target, device_id_type=MESH,
        )
        copy.start()
        return copy

    def along(device, step):
        return (xor(device[0], 2 * step), device[1])

    me = (sp, tp)
    for load in loads[:4]:
        load.wait()
    latent = jnp.dot(tokens[...], latent_down[...], preferred_element_type=F32)
    rope = nt_dot(tokens[...], rope_down[...])
    latent = norm_lanes(latent, latent_gain[...]).astype(BF16)
    rope = jnp.concatenate([rope, jnp.zeros((rows, LANES - ROPE), F32)], axis=1).astype(BF16)
    own = pl.ds(pl.multiple_of((sp * n_tp + tp) * rows, rows), rows)
    lat[own, :kvr] = latent
    lat[own, kvr:] = rope
    pl.semaphore_wait(barrier, n_outer + n_tp - 1)

    each(n_outer - 1, lambda k: send(block(me), z_send, z_recv, k, along(me, k + 1)) and None)
    send(block(me), a_send, a_recv, 0, first)
    send(block(me), b_send, b_recv, 0, second)
    send(block(me), c_send, c_recv, 0, core)

    for load in loads[4:6]:
        load.wait()
    query_latent = jnp.dot(tokens[...], query_down[...], preferred_element_type=F32)
    query_latent = norm_lanes(query_latent, query_latent_gain[...]).astype(BF16)
    own_q = pl.ds(pl.multiple_of(tp * rows, rows), rows)
    qlat[own_q, :] = query_latent
    across = (sp, xor(tp, 2))

    def query_block(index):
        return qlat.at[pl.ds(pl.multiple_of(index * rows, rows), rows)]

    send(query_block(tp), q_send, q_recv, 0, across)
    send(query_block(tp), q_send, q_recv, 1, core)

    for load in loads[6:]:
        load.wait()
    inverse = inverse_ref[...]
    query_gain_column = column(query_gain[...])
    key_gain_column = column(key_gain[...])
    ends = []
    total = 0
    for doc in range(lengths.shape[0]):
        total = total + lengths[doc]
        ends.append(total)

    def docs_of(places):
        found = jnp.zeros(places.shape, jnp.int32)
        for end in ends:
            found = found + (places >= end).astype(jnp.int32)
        return found

    seq = lat.shape[0]
    span = min(seq, KEY_CHUNK)
    query_base = sp * group_rows
    query_places = query_base + lax.broadcasted_iota(jnp.int32, (1, group_rows), 1)
    query_angles = inverse * query_places.astype(F32)
    query_cos, query_sin = jnp.cos(query_angles), jnp.sin(query_angles)
    query_docs = docs_of(query_base + lax.broadcasted_iota(jnp.int32, (group_rows, 1), 0))

    def key_tables(offset):
        places = offset + lax.broadcasted_iota(jnp.int32, (1, span), 1)
        angles = inverse * places.astype(F32)
        return jnp.cos(angles), jnp.sin(angles), docs_of(places) == query_docs

    plain_rows = head_count * NOPE
    key_up_t = jnp.transpose(key_up[...].astype(F32)).astype(BF16)
    eye = (
        lax.broadcasted_iota(jnp.int32, (ROPE, LANES), 0)
        == lax.broadcasted_iota(jnp.int32, (ROPE, LANES), 1)
    ).astype(F32).astype(BF16)
    if seq == span:
        tables = key_tables(0)

    def recv(ref, sends, recvs, index, target):
        pltpu.make_async_remote_copy(
            src_ref=ref, dst_ref=ref, send_sem=sends.at[index], recv_sem=recvs.at[index],
            device_id=target, device_id_type=MESH,
        ).wait_recv()

    def from_first(k):
        source = along(first, k)
        recv(block(source), a_send, a_recv, k, first)
        send(block(source), b_send, b_recv, 2 * k + 1, second)
        send(block(source), c_send, c_recv, 4 * k + 1, core)

    def from_z(k):
        source = along(me, k)
        recv(block(source), z_send, z_recv, k - 1, source)
        send(block(source), a_send, a_recv, k, first)
        send(block(source), b_send, b_recv, 2 * k, second)
        send(block(source), c_send, c_recv, 4 * k, core)

    def both(k):
        return along((xor(sp, 1), xor(tp, 2)), k)

    def from_second(k):
        source = along(second, k)
        recv(block(source), b_send, b_recv, 2 * k, second)
        send(block(source), c_send, c_recv, 4 * k + 2, core)

    def from_both(k):
        source = both(k)
        recv(block(source), b_send, b_recv, 2 * k + 1, second)
        send(block(source), c_send, c_recv, 4 * k + 3, core)

    from_first(0)
    from_second(0)
    recv(query_block(xor(tp, 2)), q_send, q_recv, 0, across)
    send(query_block(xor(tp, 2)), q_send, q_recv, 2, core)
    each(n_outer - 1, lambda k: from_z(k + 1))
    from_both(0)

    def rest(k):
        from_first(k + 1)
        from_second(k + 1)

    each(n_outer - 1, rest)

    recv(query_block(xor(tp, 1)), q_send, q_recv, 1, core)
    recv(query_block(xor(tp, 3)), q_send, q_recv, 2, core)
    raw = nt_dot(query_up[...], qlat[...])
    queries = []
    for head in range(head_count):
        piece = raw[head * WIDTH:(head + 1) * WIDTH]
        scale = lax.rsqrt(jnp.mean(piece * piece, axis=0, keepdims=True) + EPS)
        piece = piece * scale * query_gain_column
        piece = jnp.concatenate(
            [piece[:NOPE], rotated(piece[NOPE:], query_cos, query_sin),
             jnp.zeros((LANES - WIDTH, group_rows), F32)], axis=0
        )
        queries.append(jnp.transpose(piece)[:, :WIDTH].astype(BF16))

    each(n_outer - 1, lambda k: from_both(k + 1))

    def from_core(k):
        recv(block(along(core, k)), c_send, c_recv, 4 * k, core)
        partner_first = (xor(core[0], parity), xor(core[1], 2 * (1 - parity)))
        partner_second = (xor(core[0], 1 - parity), xor(core[1], 2 * parity))
        recv(block(along(partner_first, k)), c_send, c_recv, 4 * k + 1, core)
        recv(block(along(partner_second, k)), c_send, c_recv, 4 * k + 2, core)
        recv(block(along((xor(core[0], 1), xor(core[1], 2)), k)), c_send, c_recv, 4 * k + 3, core)

    each(n_outer, from_core)

    lane = lax.broadcasted_iota(jnp.int32, (group_rows, out_width), 1)
    score_scale = WIDTH ** (-0.5)

    def absorb(offset, known, carried):
        cosine, sine, allowed = known
        block_rows = lat[pl.ds(offset, span), :]
        latents = block_rows[:, :kvr]
        plain = nt_dot(key_up_t, latents)
        shared = nt_dot(eye, block_rows[:, kvr:])
        values = jnp.dot(latents, value_up[...], preferred_element_type=F32).astype(BF16)
        shared_square = jnp.sum(shared * shared, axis=0, keepdims=True)
        fresh = []
        for head in range(head_count):
            top, row_total, weighted = carried[head]
            part = plain[head * NOPE:(head + 1) * NOPE]
            square = jnp.sum(part * part, axis=0, keepdims=True) + shared_square
            scale = lax.rsqrt(square * (1.0 / WIDTH) + EPS)
            tail = rotated(shared * scale * key_gain_column[NOPE:], cosine, sine)
            keys = jnp.concatenate(
                [part * scale * key_gain_column[:NOPE], tail], axis=0
            ).astype(BF16)
            scores = jnp.dot(queries[head], keys, preferred_element_type=F32) * score_scale
            scores = jnp.where(allowed, scores, NEG)
            newest = jnp.maximum(top, jnp.max(scores, axis=1, keepdims=True))
            weights = jnp.where(allowed, jnp.exp(scores - newest), 0.0)
            rescale = jnp.exp(top - newest)
            row_total = row_total * rescale + jnp.sum(weights, axis=1, keepdims=True)
            weighted = weighted * rescale + jnp.dot(
                weights.astype(BF16), values, preferred_element_type=F32
            )
            fresh.append((newest, row_total, weighted))
        return tuple(fresh)

    carried = tuple(
        (jnp.full((group_rows, 1), NEG, F32), jnp.zeros((group_rows, 1), F32),
         jnp.zeros((group_rows, out_width), F32))
        for _ in range(head_count)
    )
    if seq == span:
        carried = absorb(0, tables, carried)
    else:
        def one_chunk(turn, held):
            offset = pl.multiple_of(turn * span, span)
            return absorb(offset, key_tables(offset), held)

        carried = lax.fori_loop(0, seq // span, one_chunk, carried)

    head_out = jnp.zeros((group_rows, out_width), F32)
    for head in range(head_count):
        top, row_total, weighted = carried[head]
        inside = (lane >= head * VD) & (lane < (head + 1) * VD)
        head_out = jnp.where(inside, weighted / row_total, head_out)
    heads[tp] = head_out.astype(BF16)
    for other in range(1, n_tp):
        send(heads.at[tp], h_send, h_recv, other - 1, (sp, xor(tp, other)))

    logs = jnp.concatenate(
        [jnp.broadcast_to(top + jnp.log(row_total), (group_rows, LANES // head_count))
         for top, row_total, _ in carried], axis=1
    )
    logs = jnp.transpose(logs)
    for head in range(head_count):
        start = head * (LANES // head_count)
        log_ref[head:head + 1, :] = logs[start:start + 1]

    for other in range(1, n_tp):
        peer = xor(tp, other)
        recv(heads.at[peer], h_send, h_recv, other - 1, (sp, peer))
    pieces = [heads[index].astype(F32) for index in range(n_tp)]
    square = sum(jnp.sum(piece * piece, axis=1, keepdims=True) for piece in pieces)
    scale = lax.rsqrt(square * (1.0 / (n_tp * out_width)) + EPS)
    normed = jnp.concatenate(
        [(piece * scale * output_gain[:, index * out_width:(index + 1) * out_width]).astype(BF16)
         for index, piece in enumerate(pieces)], axis=1
    )
    out_ref[...] = jnp.dot(normed, output_weight[...], preferred_element_type=F32).astype(BF16)

    def sent(ref, sends, recvs, index):
        pltpu.make_async_remote_copy(
            src_ref=ref, dst_ref=ref, send_sem=sends.at[index], recv_sem=recvs.at[index],
            device_id=core, device_id_type=MESH,
        ).wait_send()

    each(n_outer - 1, lambda k: sent(block(me), z_send, z_recv, k))
    each(n_outer, lambda k: sent(block(along(me, k)), a_send, a_recv, k))

    def sent_rest(k):
        sent(block(along(me, k)), b_send, b_recv, 2 * k)
        sent(block(along(first, k)), b_send, b_recv, 2 * k + 1)
        sent(block(along(me, k)), c_send, c_recv, 4 * k)
        sent(block(along(first, k)), c_send, c_recv, 4 * k + 1)
        sent(block(along(second, k)), c_send, c_recv, 4 * k + 2)
        sent(block(both(k)), c_send, c_recv, 4 * k + 3)

    each(n_outer, sent_rest)
    for other in range(n_tp - 1):
        sent(query_block(tp), q_send, q_recv, other)
        sent(heads.at[tp], h_send, h_recv, other)


def per_device(
    n_sp, n_tp, tokens, doc_lengths, query_down, latent_down, rope_down,
    query_latent_gain, latent_gain, query_up, key_up, value_up,
    query_gain, key_gain, output_gain, output_weight,
):
    rows = tokens.shape[0]
    group_rows = rows * n_tp
    seq = group_rows * n_sp
    half = ROPE // 2
    inverse = jnp.asarray(
        np.float32(THETA) ** (-np.arange(half, dtype=np.float32) / half), F32
    ).reshape(half, 1)
    operands = (
        tokens, doc_lengths, query_down, latent_down, rope_down.T,
        query_latent_gain[None], latent_gain[None], query_up.T, key_up, value_up,
        query_gain[None], key_gain[None], output_gain[None], output_weight, inverse,
    )
    n_outer = n_sp // 2
    head_count = key_up.shape[1] // NOPE
    kvr = latent_down.shape[1]
    held = [
        pltpu.SMEM(member.shape, member.dtype) if position == 1
        else pltpu.VMEM(member.shape, member.dtype)
        for position, member in enumerate(operands)
    ]
    dma = pltpu.SemaphoreType.DMA
    return pl.pallas_call(
        functools.partial(kernel, n_sp, n_tp),
        out_shape=(
            jax.ShapeDtypeStruct((group_rows, output_weight.shape[1]), BF16),
            jax.ShapeDtypeStruct((head_count, group_rows), F32),
        ),
        in_specs=[pl.BlockSpec(memory_space=pltpu.HBM)] * len(operands),
        out_specs=(pl.BlockSpec(memory_space=pltpu.VMEM),) * 2,
        scratch_shapes=held + [
            pltpu.VMEM((seq, kvr + LANES), BF16),
            pltpu.VMEM((group_rows, query_down.shape[1]), BF16),
            pltpu.VMEM((n_tp, group_rows, head_count * VD), BF16),
            dma((len(operands),)),
            dma((n_outer - 1,)), dma((n_outer - 1,)),
            dma((n_outer,)), dma((n_outer,)),
            dma((2 * n_outer,)), dma((2 * n_outer,)),
            dma((4 * n_outer,)), dma((4 * n_outer,)),
            dma((n_tp - 1,)), dma((n_tp - 1,)),
            dma((n_tp - 1,)), dma((n_tp - 1,)),
        ],
        compiler_params=pltpu.CompilerParams(
            collective_id=0, has_side_effects=True, vmem_limit_bytes=(16 + seq // 512) * 1024 * 1024
        ),
    )(*[pltpu.with_memory_space_constraint(member, pltpu.HBM) for member in operands])


def solution(mesh):
    n_sp, n_tp = mesh.shape["sp"], mesh.shape["tp"]
    return jax.shard_map(
        functools.partial(per_device, n_sp, n_tp),
        mesh=mesh,
        in_specs=(
            P(("sp", "tp"), None), P(), P(), P(), P(), P(), P(),
            P(None, "tp"), P(None, "tp"), P(None, "tp"),
            P(), P(), P(), P(None, "tp"),
        ),
        out_specs=(P("sp", "tp"), P("tp", "sp")),
        check_vma=False,
    )
```

```python
import functools

import jax
import jax.numpy as jnp
import numpy as np
from jax import lax
from jax.experimental import pallas as pl
from jax.experimental.pallas import tpu as pltpu
from jax.sharding import PartitionSpec as P

NOPE = 64
ROPE = 32
VD = 64
WIDTH = NOPE + ROPE
LANES = 128

EPS = 1e-06
THETA = 10000.0
NEG = -1e30
KEY_CHUNK = 1024
F32 = jnp.float32
BF16 = jnp.bfloat16
MESH = pl.DeviceIdType.MESH


def each(count, body):
    if count <= 16:
        for step in range(count):
            body(step)
    else:
        lax.fori_loop(0, count, lambda step, _: (body(step), 0)[1], 0)


def nt_dot(left, right):
    return lax.dot_general(left, right, (((1,), (1,)), ((), ())), preferred_element_type=F32)


def norm_lanes(matrix, scaling):
    mean_square = jnp.mean(matrix * matrix, axis=-1, keepdims=True)
    return matrix * lax.rsqrt(mean_square + EPS) * scaling


def column(row):
    width = row.shape[1]
    full = jnp.broadcast_to(row, (LANES, width))
    full = jnp.concatenate([full, jnp.zeros((LANES, LANES - width), F32)], axis=1)
    return jnp.transpose(full)[:width, 0:1]


def rotated(part, cosine, sine):
    half = part.shape[0] // 2
    leading, trailing = part[:half], part[half:]
    return jnp.concatenate(
        [leading * cosine - trailing * sine, trailing * cosine + leading * sine], axis=0
    )


def xor(index, bits):
    return jnp.bitwise_xor(index, bits)


def kernel(
    n_sp, n_tp,
    tokens_hbm, lengths_hbm, query_down_hbm, latent_down_hbm, rope_down_hbm,
    query_latent_gain_hbm, latent_gain_hbm, query_up_hbm, key_up_hbm, value_up_hbm,
    query_gain_hbm, key_gain_hbm, output_gain_hbm, output_weight_hbm, inverse_hbm,
    out_ref, log_ref,
    tokens, lengths, query_down, latent_down, rope_down,
    query_latent_gain, latent_gain, query_up, key_up, value_up,
    query_gain, key_gain, output_gain, output_weight, inverse_ref,
    lat, ropes, qlat, heads, load_sem,
    z_send, z_recv, a_send, a_recv, b_send, b_recv, c_send, c_recv,
    q_send, q_recv, h_send, h_recv,
):
    sp, tp = lax.axis_index("sp"), lax.axis_index("tp")
    n_outer = n_sp // 2
    rows = tokens.shape[0]
    group_rows = rows * n_tp
    kvr = latent_down.shape[1]
    head_count = key_up.shape[1] // NOPE
    out_width = head_count * VD

    loads = [
        pltpu.make_async_copy(source, target, load_sem.at[position])
        for position, (source, target) in enumerate((
            (tokens_hbm, tokens), (latent_down_hbm, latent_down), (rope_down_hbm, rope_down),
            (latent_gain_hbm, latent_gain), (query_down_hbm, query_down),
            (query_latent_gain_hbm, query_latent_gain), (lengths_hbm, lengths),
            (query_gain_hbm, query_gain), (key_gain_hbm, key_gain), (inverse_hbm, inverse_ref),
            (query_up_hbm, query_up), (key_up_hbm, key_up), (value_up_hbm, value_up),
            (output_gain_hbm, output_gain), (output_weight_hbm, output_weight),
        ))
    ]
    for load in loads:
        load.start()

    barrier = pltpu.get_barrier_semaphore()

    def greet(step):
        pl.semaphore_signal(
            barrier, inc=1, device_id=(xor(sp, 2 * (step + 1)), tp), device_id_type=MESH
        )

    each(n_outer - 1, greet)
    pl.semaphore_signal(barrier, inc=1, device_id=(xor(sp, 1), tp), device_id_type=MESH)
    for other in range(1, n_tp):
        pl.semaphore_signal(barrier, inc=1, device_id=(sp, xor(tp, other)), device_id_type=MESH)

    parity = lax.rem(tp, 2)
    first = (xor(sp, 1 - parity), xor(tp, 2 * parity))
    second = (xor(sp, parity), xor(tp, 2 * (1 - parity)))
    core = (sp, xor(tp, 1))

    def block(device):
        place = device[0] * n_tp + device[1]
        return lat.at[pl.ds(pl.multiple_of(place * rows, rows), rows)], ropes.at[place]

    def copies(ref, sends, recvs, index, target):
        if not isinstance(ref, tuple):
            ref, index = (ref,), ((index,),)
        else:
            index = tuple((part, index) for part in range(len(ref)))
        return [
            pltpu.make_async_remote_copy(
                src_ref=part, dst_ref=part, send_sem=sends.at[place], recv_sem=recvs.at[place],
                device_id=target, device_id_type=MESH,
            )
            for part, place in zip(ref, index)
        ]

    def send(ref, sends, recvs, index, target):
        for copy in copies(ref, sends, recvs, index, target):
            copy.start()

    def recv(ref, sends, recvs, index, target):
        for copy in copies(ref, sends, recvs, index, target):
            copy.wait_recv()

    def sent(ref, sends, recvs, index):
        for copy in copies(ref, sends, recvs, index, core):
            copy.wait_send()

    def along(device, step):
        return (xor(device[0], 2 * step), device[1])

    me = (sp, tp)
    for load in loads[:4]:
        load.wait()
    latent = jnp.dot(tokens[...], latent_down[...], preferred_element_type=F32)
    rope = nt_dot(rope_down[...], tokens[...])
    latent = norm_lanes(latent, latent_gain[...]).astype(BF16)
    rope = jnp.concatenate(
        [rope[start:start + 8] for start in range(0, ROPE, 8)], axis=1
    ).astype(BF16)
    own = pl.ds(pl.multiple_of((sp * n_tp + tp) * rows, rows), rows)
    lat[own, :] = latent
    ropes[sp * n_tp + tp] = rope
    pl.semaphore_wait(barrier, n_outer + n_tp - 1)

    each(n_outer - 1, lambda k: send(block(me), z_send, z_recv, k, along(me, k + 1)))
    send(block(me), a_send, a_recv, 0, first)
    send(block(me), b_send, b_recv, 0, second)
    send(block(me), c_send, c_recv, 0, core)

    for load in loads[4:6]:
        load.wait()
    query_latent = jnp.dot(tokens[...], query_down[...], preferred_element_type=F32)
    query_latent = norm_lanes(query_latent, query_latent_gain[...]).astype(BF16)
    own_q = pl.ds(pl.multiple_of(tp * rows, rows), rows)
    qlat[own_q, :] = query_latent
    across = (sp, xor(tp, 2))

    def query_block(index):
        return qlat.at[pl.ds(pl.multiple_of(index * rows, rows), rows)]

    send(query_block(tp), q_send, q_recv, 0, across)
    send(query_block(tp), q_send, q_recv, 1, core)

    for load in loads[6:]:
        load.wait()
    inverse = inverse_ref[...]
    query_gain_column = column(query_gain[...])
    key_gain_column = column(key_gain[...])
    ends = []
    total = 0
    for doc in range(lengths.shape[0]):
        total = total + lengths[doc]
        ends.append(total)

    def docs_of(places):
        found = jnp.zeros(places.shape, jnp.int32)
        for end in ends:
            found = found + (places >= end).astype(jnp.int32)
        return found

    seq = lat.shape[0]
    span = min(seq, KEY_CHUNK)
    query_base = sp * group_rows
    query_places = query_base + lax.broadcasted_iota(jnp.int32, (1, group_rows), 1)

    def key_tables(offset):
        places = offset + lax.broadcasted_iota(jnp.int32, (1, span), 1)
        angles = inverse * places.astype(F32)
        return jnp.cos(angles), jnp.sin(angles), docs_of(places) == query_docs

    plain_rows = head_count * NOPE
    key_up_t = jnp.transpose(key_up[...].astype(F32)).astype(BF16)
    def from_first(k):
        source = along(first, k)
        recv(block(source), a_send, a_recv, k, first)
        send(block(source), b_send, b_recv, 2 * k + 1, second)
        send(block(source), c_send, c_recv, 4 * k + 1, core)

    def from_z(k):
        source = along(me, k)
        recv(block(source), z_send, z_recv, k - 1, source)
        send(block(source), a_send, a_recv, k, first)
        send(block(source), b_send, b_recv, 2 * k, second)
        send(block(source), c_send, c_recv, 4 * k, core)

    def both(k):
        return along((xor(sp, 1), xor(tp, 2)), k)

    def from_second(k):
        source = along(second, k)
        recv(block(source), b_send, b_recv, 2 * k, second)
        send(block(source), c_send, c_recv, 4 * k + 2, core)

    def from_both(k):
        source = both(k)
        recv(block(source), b_send, b_recv, 2 * k + 1, second)
        send(block(source), c_send, c_recv, 4 * k + 3, core)

    from_first(0)
    from_second(0)
    recv(query_block(xor(tp, 2)), q_send, q_recv, 0, across)
    send(query_block(xor(tp, 2)), q_send, q_recv, 2, core)
    each(n_outer - 1, lambda k: from_z(k + 1))
    from_both(0)
    each(n_outer - 1, lambda k: from_first(k + 1))
    query_angles = inverse * query_places.astype(F32)
    query_cos, query_sin = jnp.cos(query_angles), jnp.sin(query_angles)
    query_docs = docs_of(query_base + lax.broadcasted_iota(jnp.int32, (group_rows, 1), 0))
    if seq == span:
        tables = key_tables(0)

    recv(query_block(xor(tp, 1)), q_send, q_recv, 1, core)
    recv(query_block(xor(tp, 3)), q_send, q_recv, 2, core)
    raw = nt_dot(query_up[...], qlat[...])
    queries = []
    for head in range(head_count):
        piece = raw[head * WIDTH:(head + 1) * WIDTH]
        scale = lax.rsqrt(jnp.mean(piece * piece, axis=0, keepdims=True) + EPS)
        piece = piece * scale * query_gain_column
        piece = jnp.concatenate(
            [piece[:NOPE], rotated(piece[NOPE:], query_cos, query_sin),
             jnp.zeros((LANES - WIDTH, group_rows), F32)], axis=0
        )
        queries.append(jnp.transpose(piece)[:, :WIDTH].astype(BF16))

    each(n_outer - 1, lambda k: from_second(k + 1))
    each(n_outer - 1, lambda k: from_both(k + 1))

    def from_core(k):
        recv(block(along(core, k)), c_send, c_recv, 4 * k, core)
        partner_first = (xor(core[0], parity), xor(core[1], 2 * (1 - parity)))
        partner_second = (xor(core[0], 1 - parity), xor(core[1], 2 * parity))
        recv(block(along(partner_first, k)), c_send, c_recv, 4 * k + 1, core)
        recv(block(along(partner_second, k)), c_send, c_recv, 4 * k + 2, core)
        recv(block(along((xor(core[0], 1), xor(core[1], 2)), k)), c_send, c_recv, 4 * k + 3, core)

    each(n_outer, from_core)

    lane = lax.broadcasted_iota(jnp.int32, (group_rows, out_width), 1)
    score_scale = WIDTH ** (-0.5)

    def unpacked(offset):
        groups = ROPE // 8
        lanes = groups * rows
        segment = lax.broadcasted_iota(jnp.int32, (8, lanes), 1) // rows
        base = offset // rows
        columns = []
        for start in range(0, span // rows, groups):
            packed = [ropes[base + start + place].astype(F32) for place in range(groups)]
            bands = []
            for group in range(groups):
                band = packed[group]
                for place in range(groups):
                    if place != group:
                        shift = ((place - group) * rows) % lanes
                        moved = pltpu.roll(packed[place], shift, 1)
                        band = jnp.where(segment == place, moved, band)
                bands.append(band)
            columns.append(jnp.concatenate(bands, axis=0))
        return jnp.concatenate(columns, axis=1)

    def absorb(offset, known, carried):
        cosine, sine, allowed = known
        latents = lat[pl.ds(offset, span), :]
        plain = nt_dot(key_up_t, latents)
        shared = unpacked(offset)
        values = jnp.dot(latents, value_up[...], preferred_element_type=F32).astype(BF16)
        shared_square = jnp.sum(shared * shared, axis=0, keepdims=True)
        fresh = []
        for head in range(head_count):
            top, row_total, weighted = carried[head]
            part = plain[head * NOPE:(head + 1) * NOPE]
            square = jnp.sum(part * part, axis=0, keepdims=True) + shared_square
            scale = lax.rsqrt(square * (1.0 / WIDTH) + EPS)
            tail = rotated(shared * scale * key_gain_column[NOPE:], cosine, sine)
            keys = jnp.concatenate(
                [part * scale * key_gain_column[:NOPE], tail], axis=0
            ).astype(BF16)
            scores = jnp.dot(queries[head], keys, preferred_element_type=F32) * score_scale
            scores = jnp.where(allowed, scores, NEG)
            newest = jnp.maximum(top, jnp.max(scores, axis=1, keepdims=True))
            weights = jnp.where(allowed, jnp.exp(scores - newest), 0.0)
            rescale = jnp.exp(top - newest)
            row_total = row_total * rescale + jnp.sum(weights, axis=1, keepdims=True)
            weighted = weighted * rescale + jnp.dot(
                weights.astype(BF16), values, preferred_element_type=F32
            )
            fresh.append((newest, row_total, weighted))
        return tuple(fresh)

    carried = tuple(
        (jnp.full((group_rows, 1), NEG, F32), jnp.zeros((group_rows, 1), F32),
         jnp.zeros((group_rows, out_width), F32))
        for _ in range(head_count)
    )
    if seq == span:
        carried = absorb(0, tables, carried)
    else:
        def one_chunk(turn, held):
            offset = pl.multiple_of(turn * span, span)
            return absorb(offset, key_tables(offset), held)

        carried = lax.fori_loop(0, seq // span, one_chunk, carried)

    head_out = jnp.zeros((group_rows, out_width), F32)
    for head in range(head_count):
        top, row_total, weighted = carried[head]
        inside = (lane >= head * VD) & (lane < (head + 1) * VD)
        head_out = jnp.where(inside, weighted / row_total, head_out)
    heads[tp] = head_out.astype(BF16)
    for other in range(1, n_tp):
        send(heads.at[tp], h_send, h_recv, other - 1, (sp, xor(tp, other)))

    logs = jnp.concatenate(
        [jnp.broadcast_to(top + jnp.log(row_total), (group_rows, LANES // head_count))
         for top, row_total, _ in carried], axis=1
    )
    logs = jnp.transpose(logs)
    for head in range(head_count):
        start = head * (LANES // head_count)
        log_ref[head:head + 1, :] = logs[start:start + 1]

    for other in range(1, n_tp):
        peer = xor(tp, other)
        recv(heads.at[peer], h_send, h_recv, other - 1, (sp, peer))
    pieces = [heads[index].astype(F32) for index in range(n_tp)]
    square = sum(jnp.sum(piece * piece, axis=1, keepdims=True) for piece in pieces)
    scale = lax.rsqrt(square * (1.0 / (n_tp * out_width)) + EPS)
    normed = jnp.concatenate(
        [(piece * scale * output_gain[:, index * out_width:(index + 1) * out_width]).astype(BF16)
         for index, piece in enumerate(pieces)], axis=1
    )
    out_ref[...] = jnp.dot(normed, output_weight[...], preferred_element_type=F32).astype(BF16)

    each(n_outer - 1, lambda k: sent(block(me), z_send, z_recv, k))
    each(n_outer, lambda k: sent(block(along(me, k)), a_send, a_recv, k))

    def sent_rest(k):
        sent(block(along(me, k)), b_send, b_recv, 2 * k)
        sent(block(along(first, k)), b_send, b_recv, 2 * k + 1)
        sent(block(along(me, k)), c_send, c_recv, 4 * k)
        sent(block(along(first, k)), c_send, c_recv, 4 * k + 1)
        sent(block(along(second, k)), c_send, c_recv, 4 * k + 2)
        sent(block(both(k)), c_send, c_recv, 4 * k + 3)

    each(n_outer, sent_rest)
    for other in range(n_tp - 1):
        sent(query_block(tp), q_send, q_recv, other)
        sent(heads.at[tp], h_send, h_recv, other)


def per_device(
    n_sp, n_tp, tokens, doc_lengths, query_down, latent_down, rope_down,
    query_latent_gain, latent_gain, query_up, key_up, value_up,
    query_gain, key_gain, output_gain, output_weight,
):
    rows = tokens.shape[0]
    group_rows = rows * n_tp
    seq = group_rows * n_sp
    half = ROPE // 2
    inverse = jnp.asarray(
        np.float32(THETA) ** (-np.arange(half, dtype=np.float32) / half), F32
    ).reshape(half, 1)
    operands = (
        tokens, doc_lengths, query_down, latent_down, rope_down.T,
        query_latent_gain[None], latent_gain[None], query_up.T, key_up, value_up,
        query_gain[None], key_gain[None], output_gain[None], output_weight, inverse,
    )
    n_outer = n_sp // 2
    head_count = key_up.shape[1] // NOPE
    kvr = latent_down.shape[1]
    held = [
        pltpu.SMEM(member.shape, member.dtype) if position == 1
        else pltpu.VMEM(member.shape, member.dtype)
        for position, member in enumerate(operands)
    ]
    dma = pltpu.SemaphoreType.DMA
    return pl.pallas_call(
        functools.partial(kernel, n_sp, n_tp),
        out_shape=(
            jax.ShapeDtypeStruct((group_rows, output_weight.shape[1]), BF16),
            jax.ShapeDtypeStruct((head_count, group_rows), F32),
        ),
        in_specs=[pl.BlockSpec(memory_space=pltpu.HBM)] * len(operands),
        out_specs=(pl.BlockSpec(memory_space=pltpu.VMEM),) * 2,
        scratch_shapes=held + [
            pltpu.VMEM((seq, kvr), BF16),
            pltpu.VMEM((seq // rows, 8, ROPE * rows // 8), BF16),
            pltpu.VMEM((group_rows, query_down.shape[1]), BF16),
            pltpu.VMEM((n_tp, group_rows, head_count * VD), BF16),
            dma((len(operands),)),
            dma((2, n_outer - 1)), dma((2, n_outer - 1)),
            dma((2, n_outer)), dma((2, n_outer)),
            dma((2, 2 * n_outer)), dma((2, 2 * n_outer)),
            dma((2, 4 * n_outer)), dma((2, 4 * n_outer)),
            dma((n_tp - 1,)), dma((n_tp - 1,)),
            dma((n_tp - 1,)), dma((n_tp - 1,)),
        ],
        compiler_params=pltpu.CompilerParams(
            collective_id=0, has_side_effects=True, vmem_limit_bytes=(16 + seq // 512) * 1024 * 1024
        ),
    )(*[pltpu.with_memory_space_constraint(member, pltpu.HBM) for member in operands])


def solution(mesh):
    n_sp, n_tp = mesh.shape["sp"], mesh.shape["tp"]
    return jax.shard_map(
        functools.partial(per_device, n_sp, n_tp),
        mesh=mesh,
        in_specs=(
            P(("sp", "tp"), None), P(), P(), P(), P(), P(), P(),
            P(None, "tp"), P(None, "tp"), P(None, "tp"),
            P(), P(), P(), P(None, "tp"),
        ),
        out_specs=(P("sp", "tp"), P("tp", "sp")),
        check_vma=False,
    )
```

```python
import functools

import jax
import jax.numpy as jnp
import numpy as np
from jax import lax
from jax.experimental import pallas as pl
from jax.experimental.pallas import tpu as pltpu
from jax.sharding import PartitionSpec as P

NOPE = 64
ROPE = 32
VD = 64
WIDTH = NOPE + ROPE
LANES = 128

EPS = 1e-06
THETA = 10000.0
NEG = -1e30
KEY_CHUNK = 1024
F32 = jnp.float32
BF16 = jnp.bfloat16
MESH = pl.DeviceIdType.MESH


def each(count, body):
    if count <= 16:
        for step in range(count):
            body(step)
    else:
        lax.fori_loop(0, count, lambda step, _: (body(step), 0)[1], 0)


def nt_dot(left, right):
    return lax.dot_general(left, right, (((1,), (1,)), ((), ())), preferred_element_type=F32)


def norm_lanes(matrix, scaling):
    mean_square = jnp.mean(matrix * matrix, axis=-1, keepdims=True)
    return matrix * lax.rsqrt(mean_square + EPS) * scaling


def column(row):
    width = row.shape[1]
    full = jnp.broadcast_to(row, (LANES, width))
    full = jnp.concatenate([full, jnp.zeros((LANES, LANES - width), F32)], axis=1)
    return jnp.transpose(full)[:width, 0:1]


def rotated(part, cosine, sine):
    half = part.shape[0] // 2
    leading, trailing = part[:half], part[half:]
    return jnp.concatenate(
        [leading * cosine - trailing * sine, trailing * cosine + leading * sine], axis=0
    )


def xor(index, bits):
    return jnp.bitwise_xor(index, bits)


def kernel(
    n_sp, n_tp,
    tokens_hbm, lengths_hbm, query_down_hbm, latent_down_hbm, rope_down_hbm,
    query_latent_gain_hbm, latent_gain_hbm, query_up_hbm, key_up_hbm, value_up_hbm,
    query_gain_hbm, key_gain_hbm, output_gain_hbm, output_weight_hbm, inverse_hbm,
    out_ref, log_ref,
    tokens, lengths, query_down, latent_down, rope_down,
    query_latent_gain, latent_gain, query_up, key_up, value_up,
    query_gain, key_gain, output_gain, output_weight, inverse_ref,
    lat, ropes, qlat, heads, load_sem,
    z_send, z_recv, a_send, a_recv, b_send, b_recv, c_send, c_recv,
    q_send, q_recv, h_send, h_recv,
):
    sp, tp = lax.axis_index("sp"), lax.axis_index("tp")
    n_outer = n_sp // 2
    rows = tokens.shape[0]
    group_rows = rows * n_tp
    kvr = latent_down.shape[1]
    head_count = key_up.shape[1] // NOPE
    out_width = head_count * VD

    loads = [
        pltpu.make_async_copy(source, target, load_sem.at[position])
        for position, (source, target) in enumerate((
            (tokens_hbm, tokens), (latent_down_hbm, latent_down), (rope_down_hbm, rope_down),
            (latent_gain_hbm, latent_gain), (query_down_hbm, query_down),
            (query_latent_gain_hbm, query_latent_gain), (lengths_hbm, lengths),
            (query_gain_hbm, query_gain), (key_gain_hbm, key_gain), (inverse_hbm, inverse_ref),
            (query_up_hbm, query_up), (key_up_hbm, key_up), (value_up_hbm, value_up),
            (output_gain_hbm, output_gain), (output_weight_hbm, output_weight),
        ))
    ]
    for load in loads:
        load.start()

    barrier = pltpu.get_barrier_semaphore()

    def greet(step):
        pl.semaphore_signal(
            barrier, inc=1, device_id=(xor(sp, 2 * (step + 1)), tp), device_id_type=MESH
        )

    each(n_outer - 1, greet)
    pl.semaphore_signal(barrier, inc=1, device_id=(xor(sp, 1), tp), device_id_type=MESH)
    pl.semaphore_signal(
        barrier, inc=1, device_id=(xor(sp, 1), xor(tp, 2)), device_id_type=MESH
    )
    for other in range(1, n_tp):
        pl.semaphore_signal(barrier, inc=1, device_id=(sp, xor(tp, other)), device_id_type=MESH)

    parity = lax.rem(tp, 2)
    first = (xor(sp, 1 - parity), xor(tp, 2 * parity))
    second = (xor(sp, parity), xor(tp, 2 * (1 - parity)))
    core = (sp, xor(tp, 1))
    corner = (xor(sp, 1), xor(tp, 2))

    def block(device):
        place = device[0] * n_tp + device[1]
        return lat.at[pl.ds(pl.multiple_of(place * rows, rows), rows)], ropes.at[place]

    def copies(ref, sends, recvs, index, target):
        if not isinstance(ref, tuple):
            ref, index = (ref,), ((index,),)
        else:
            index = tuple((part, index) for part in range(len(ref)))
        return [
            pltpu.make_async_remote_copy(
                src_ref=part, dst_ref=part, send_sem=sends.at[place], recv_sem=recvs.at[place],
                device_id=target, device_id_type=MESH,
            )
            for part, place in zip(ref, index)
        ]

    def send(ref, sends, recvs, index, target):
        for copy in copies(ref, sends, recvs, index, target):
            copy.start()

    def recv(ref, sends, recvs, index, target):
        for copy in copies(ref, sends, recvs, index, target):
            copy.wait_recv()

    def sent(ref, sends, recvs, index):
        for copy in copies(ref, sends, recvs, index, core):
            copy.wait_send()

    def along(device, step):
        return (xor(device[0], 2 * step), device[1])

    me = (sp, tp)
    for load in loads[:4]:
        load.wait()
    latent = jnp.dot(tokens[...], latent_down[...], preferred_element_type=F32)
    rope = nt_dot(rope_down[...], tokens[...])
    latent = norm_lanes(latent, latent_gain[...]).astype(BF16)
    rope = jnp.concatenate(
        [rope[start:start + 8] for start in range(0, ROPE, 8)], axis=1
    ).astype(BF16)
    own = pl.ds(pl.multiple_of((sp * n_tp + tp) * rows, rows), rows)
    lat[own, :] = latent
    ropes[sp * n_tp + tp] = rope
    pl.semaphore_wait(barrier, n_outer + n_tp)

    each(n_outer - 1, lambda k: send(block(me), z_send, z_recv, k, along(me, k + 1)))
    send(block(me), a_send, a_recv, 0, first)
    send(block(me), b_send, b_recv, 0, second)
    send(block(me), b_send, b_recv, 1, corner)
    send(block(me), c_send, c_recv, 0, core)

    for load in loads[4:6]:
        load.wait()
    query_latent = jnp.dot(tokens[...], query_down[...], preferred_element_type=F32)
    query_latent = norm_lanes(query_latent, query_latent_gain[...]).astype(BF16)
    own_q = pl.ds(pl.multiple_of(tp * rows, rows), rows)
    qlat[own_q, :] = query_latent
    across = (sp, xor(tp, 2))

    def query_block(index):
        return qlat.at[pl.ds(pl.multiple_of(index * rows, rows), rows)]

    send(query_block(tp), q_send, q_recv, 0, across)
    send(query_block(tp), q_send, q_recv, 1, core)

    for load in loads[6:]:
        load.wait()
    inverse = inverse_ref[...]
    query_gain_column = column(query_gain[...])
    key_gain_column = column(key_gain[...])
    ends = []
    total = 0
    for doc in range(lengths.shape[0]):
        total = total + lengths[doc]
        ends.append(total)

    def docs_of(places):
        found = jnp.zeros(places.shape, jnp.int32)
        for end in ends:
            found = found + (places >= end).astype(jnp.int32)
        return found

    seq = lat.shape[0]
    span = min(seq, KEY_CHUNK)
    query_base = sp * group_rows
    query_places = query_base + lax.broadcasted_iota(jnp.int32, (1, group_rows), 1)

    def key_tables(offset):
        places = offset + lax.broadcasted_iota(jnp.int32, (1, span), 1)
        angles = inverse * places.astype(F32)
        return jnp.cos(angles), jnp.sin(angles), docs_of(places) == query_docs

    plain_rows = head_count * NOPE
    key_up_t = jnp.transpose(key_up[...].astype(F32)).astype(BF16)
    def from_first(k):
        source = along(first, k)
        recv(block(source), a_send, a_recv, k, first)
        send(block(source), c_send, c_recv, 4 * k + 1, core)

    def from_z(k):
        source = along(me, k)
        recv(block(source), z_send, z_recv, k - 1, source)
        send(block(source), a_send, a_recv, k, first)
        send(block(source), b_send, b_recv, 2 * k, second)
        send(block(source), b_send, b_recv, 2 * k + 1, corner)
        send(block(source), c_send, c_recv, 4 * k, core)

    def both(k):
        return along((xor(sp, 1), xor(tp, 2)), k)

    def from_second(k):
        source = along(second, k)
        recv(block(source), b_send, b_recv, 2 * k, second)
        send(block(source), c_send, c_recv, 4 * k + 2, core)

    def from_both(k):
        source = both(k)
        recv(block(source), b_send, b_recv, 2 * k + 1, corner)
        send(block(source), c_send, c_recv, 4 * k + 3, core)

    from_first(0)
    from_second(0)
    recv(query_block(xor(tp, 2)), q_send, q_recv, 0, across)
    send(query_block(xor(tp, 2)), q_send, q_recv, 2, core)
    each(n_outer - 1, lambda k: from_z(k + 1))
    from_both(0)
    each(n_outer - 1, lambda k: from_first(k + 1))
    query_angles = inverse * query_places.astype(F32)
    query_cos, query_sin = jnp.cos(query_angles), jnp.sin(query_angles)
    query_docs = docs_of(query_base + lax.broadcasted_iota(jnp.int32, (group_rows, 1), 0))
    if seq == span:
        tables = key_tables(0)

    recv(query_block(xor(tp, 1)), q_send, q_recv, 1, core)
    recv(query_block(xor(tp, 3)), q_send, q_recv, 2, core)
    raw = nt_dot(query_up[...], qlat[...])
    queries = []
    for head in range(head_count):
        piece = raw[head * WIDTH:(head + 1) * WIDTH]
        scale = lax.rsqrt(jnp.mean(piece * piece, axis=0, keepdims=True) + EPS)
        piece = piece * scale * query_gain_column
        piece = jnp.concatenate(
            [piece[:NOPE], rotated(piece[NOPE:], query_cos, query_sin),
             jnp.zeros((LANES - WIDTH, group_rows), F32)], axis=0
        )
        queries.append(jnp.transpose(piece)[:, :WIDTH].astype(BF16))

    each(n_outer - 1, lambda k: from_second(k + 1))
    each(n_outer - 1, lambda k: from_both(k + 1))

    def from_core(k):
        recv(block(along(core, k)), c_send, c_recv, 4 * k, core)
        partner_first = (xor(core[0], parity), xor(core[1], 2 * (1 - parity)))
        partner_second = (xor(core[0], 1 - parity), xor(core[1], 2 * parity))
        recv(block(along(partner_first, k)), c_send, c_recv, 4 * k + 1, core)
        recv(block(along(partner_second, k)), c_send, c_recv, 4 * k + 2, core)
        recv(block(along((xor(core[0], 1), xor(core[1], 2)), k)), c_send, c_recv, 4 * k + 3, core)

    each(n_outer, from_core)

    lane = lax.broadcasted_iota(jnp.int32, (group_rows, out_width), 1)
    score_scale = WIDTH ** (-0.5)

    def unpacked(offset):
        groups = ROPE // 8
        lanes = groups * rows
        segment = lax.broadcasted_iota(jnp.int32, (8, lanes), 1) // rows
        base = offset // rows
        columns = []
        for start in range(0, span // rows, groups):
            packed = [ropes[base + start + place].astype(F32) for place in range(groups)]
            bands = []
            for group in range(groups):
                band = packed[group]
                for place in range(groups):
                    if place != group:
                        shift = ((place - group) * rows) % lanes
                        moved = pltpu.roll(packed[place], shift, 1)
                        band = jnp.where(segment == place, moved, band)
                bands.append(band)
            columns.append(jnp.concatenate(bands, axis=0))
        return jnp.concatenate(columns, axis=1)

    def absorb(offset, known, carried):
        cosine, sine, allowed = known
        latents = lat[pl.ds(offset, span), :]
        plain = nt_dot(key_up_t, latents)
        shared = unpacked(offset)
        values = jnp.dot(latents, value_up[...], preferred_element_type=F32).astype(BF16)
        shared_square = jnp.sum(shared * shared, axis=0, keepdims=True)
        fresh = []
        for head in range(head_count):
            top, row_total, weighted = carried[head]
            part = plain[head * NOPE:(head + 1) * NOPE]
            square = jnp.sum(part * part, axis=0, keepdims=True) + shared_square
            scale = lax.rsqrt(square * (1.0 / WIDTH) + EPS)
            tail = rotated(shared * scale * key_gain_column[NOPE:], cosine, sine)
            keys = jnp.concatenate(
                [part * scale * key_gain_column[:NOPE], tail], axis=0
            ).astype(BF16)
            scores = jnp.dot(queries[head], keys, preferred_element_type=F32) * score_scale
            scores = jnp.where(allowed, scores, NEG)
            newest = jnp.maximum(top, jnp.max(scores, axis=1, keepdims=True))
            weights = jnp.where(allowed, jnp.exp(scores - newest), 0.0)
            rescale = jnp.exp(top - newest)
            row_total = row_total * rescale + jnp.sum(weights, axis=1, keepdims=True)
            weighted = weighted * rescale + jnp.dot(
                weights.astype(BF16), values, preferred_element_type=F32
            )
            fresh.append((newest, row_total, weighted))
        return tuple(fresh)

    carried = tuple(
        (jnp.full((group_rows, 1), NEG, F32), jnp.zeros((group_rows, 1), F32),
         jnp.zeros((group_rows, out_width), F32))
        for _ in range(head_count)
    )
    if seq == span:
        carried = absorb(0, tables, carried)
    else:
        def one_chunk(turn, held):
            offset = pl.multiple_of(turn * span, span)
            return absorb(offset, key_tables(offset), held)

        carried = lax.fori_loop(0, seq // span, one_chunk, carried)

    head_out = jnp.zeros((group_rows, out_width), F32)
    for head in range(head_count):
        top, row_total, weighted = carried[head]
        inside = (lane >= head * VD) & (lane < (head + 1) * VD)
        head_out = jnp.where(inside, weighted / row_total, head_out)
    heads[tp] = head_out.astype(BF16)
    for other in range(1, n_tp):
        send(heads.at[tp], h_send, h_recv, other - 1, (sp, xor(tp, other)))

    logs = jnp.concatenate(
        [jnp.broadcast_to(top + jnp.log(row_total), (group_rows, LANES // head_count))
         for top, row_total, _ in carried], axis=1
    )
    logs = jnp.transpose(logs)
    for head in range(head_count):
        start = head * (LANES // head_count)
        log_ref[head:head + 1, :] = logs[start:start + 1]

    for other in range(1, n_tp):
        peer = xor(tp, other)
        recv(heads.at[peer], h_send, h_recv, other - 1, (sp, peer))
    pieces = [heads[index].astype(F32) for index in range(n_tp)]
    square = sum(jnp.sum(piece * piece, axis=1, keepdims=True) for piece in pieces)
    scale = lax.rsqrt(square * (1.0 / (n_tp * out_width)) + EPS)
    normed = jnp.concatenate(
        [(piece * scale * output_gain[:, index * out_width:(index + 1) * out_width]).astype(BF16)
         for index, piece in enumerate(pieces)], axis=1
    )
    out_ref[...] = jnp.dot(normed, output_weight[...], preferred_element_type=F32).astype(BF16)

    each(n_outer - 1, lambda k: sent(block(me), z_send, z_recv, k))
    each(n_outer, lambda k: sent(block(along(me, k)), a_send, a_recv, k))

    def sent_rest(k):
        sent(block(along(me, k)), b_send, b_recv, 2 * k)
        sent(block(along(me, k)), b_send, b_recv, 2 * k + 1)
        sent(block(along(me, k)), c_send, c_recv, 4 * k)
        sent(block(along(first, k)), c_send, c_recv, 4 * k + 1)
        sent(block(along(second, k)), c_send, c_recv, 4 * k + 2)
        sent(block(both(k)), c_send, c_recv, 4 * k + 3)

    each(n_outer, sent_rest)
    for other in range(n_tp - 1):
        sent(query_block(tp), q_send, q_recv, other)
        sent(heads.at[tp], h_send, h_recv, other)


def per_device(
    n_sp, n_tp, tokens, doc_lengths, query_down, latent_down, rope_down,
    query_latent_gain, latent_gain, query_up, key_up, value_up,
    query_gain, key_gain, output_gain, output_weight,
):
    rows = tokens.shape[0]
    group_rows = rows * n_tp
    seq = group_rows * n_sp
    half = ROPE // 2
    inverse = jnp.asarray(
        np.float32(THETA) ** (-np.arange(half, dtype=np.float32) / half), F32
    ).reshape(half, 1)
    operands = (
        tokens, doc_lengths, query_down, latent_down, rope_down.T,
        query_latent_gain[None], latent_gain[None], query_up.T, key_up, value_up,
        query_gain[None], key_gain[None], output_gain[None], output_weight, inverse,
    )
    n_outer = n_sp // 2
    head_count = key_up.shape[1] // NOPE
    kvr = latent_down.shape[1]
    held = [
        pltpu.SMEM(member.shape, member.dtype) if position == 1
        else pltpu.VMEM(member.shape, member.dtype)
        for position, member in enumerate(operands)
    ]
    dma = pltpu.SemaphoreType.DMA
    return pl.pallas_call(
        functools.partial(kernel, n_sp, n_tp),
        out_shape=(
            jax.ShapeDtypeStruct((group_rows, output_weight.shape[1]), BF16),
            jax.ShapeDtypeStruct((head_count, group_rows), F32),
        ),
        in_specs=[pl.BlockSpec(memory_space=pltpu.HBM)] * len(operands),
        out_specs=(pl.BlockSpec(memory_space=pltpu.VMEM),) * 2,
        scratch_shapes=held + [
            pltpu.VMEM((seq, kvr), BF16),
            pltpu.VMEM((seq // rows, 8, ROPE * rows // 8), BF16),
            pltpu.VMEM((group_rows, query_down.shape[1]), BF16),
            pltpu.VMEM((n_tp, group_rows, head_count * VD), BF16),
            dma((len(operands),)),
            dma((2, n_outer - 1)), dma((2, n_outer - 1)),
            dma((2, n_outer)), dma((2, n_outer)),
            dma((2, 2 * n_outer)), dma((2, 2 * n_outer)),
            dma((2, 4 * n_outer)), dma((2, 4 * n_outer)),
            dma((n_tp - 1,)), dma((n_tp - 1,)),
            dma((n_tp - 1,)), dma((n_tp - 1,)),
        ],
        compiler_params=pltpu.CompilerParams(
            collective_id=0, has_side_effects=True, vmem_limit_bytes=(16 + seq // 512) * 1024 * 1024
        ),
    )(*[pltpu.with_memory_space_constraint(member, pltpu.HBM) for member in operands])


def solution(mesh):
    n_sp, n_tp = mesh.shape["sp"], mesh.shape["tp"]
    return jax.shard_map(
        functools.partial(per_device, n_sp, n_tp),
        mesh=mesh,
        in_specs=(
            P(("sp", "tp"), None), P(), P(), P(), P(), P(), P(),
            P(None, "tp"), P(None, "tp"), P(None, "tp"),
            P(), P(), P(), P(None, "tp"),
        ),
        out_specs=(P("sp", "tp"), P("tp", "sp")),
        check_vma=False,
    )
```
